32 devices in a mesh: ep: 16 (over z, x, core), tp: 2 (over y).
Axes of the slice: x: 2, y: 2, z: 4, core: 2. Of those that a mesh axis runs over, the one named last changes fastest.
Arguments:
- tokens: bfloat16 [384, 2048], P('ep'), may hold values from -6 to 6
- carried_state: float32 [384, 4, 128, 128], P('ep', 'tp'), may hold values from -4 to 4
- w_query: bfloat16 [2048, 512], P(None, 'tp'), may hold values from -0.125 to 0.125
- w_forget: bfloat16 [2048, 512], P(None, 'tp'), may hold values from -0.125 to 0.125
- w_value: bfloat16 [2048, 512], P(None, 'tp'), may hold values from -0.125 to 0.125
- forget_floor: float32 [4, 128], P('tp'), may hold values from 0.05 to 0.9
- head_gain: bfloat16 [4, 128], P('tp'), may hold values from 0.099609375 to 1.8984375
- w_out: bfloat16 [512, 2048], P('tp', 'ep'), may hold values from -0.25 to 0.25
- gain_mix: bfloat16 [2048], replicated, may hold values from 0.099609375 to 1.8984375
- gain_ffn: bfloat16 [2048], replicated, may hold values from 0.099609375 to 1.8984375
- gain_post: bfloat16 [2048], P('tp'), may hold values from 0.099609375 to 1.8984375
- w_branch_gate: bfloat16 [2048], replicated, may hold values from -0.125 to 0.125
- shared_gate: bfloat16 [2048, 512], P('ep', 'tp'), may hold values from -0.125 to 0.125
- shared_up: bfloat16 [2048, 512], P('ep', 'tp'), may hold values from -0.125 to 0.125
- shared_down: bfloat16 [512, 2048], P('tp', 'ep'), may hold values from -1.1048543 to 1.1048543
- routes: int32 [384, 6], P('ep'), may hold values from 0 to 15, all different within a row; in each aligned block of 24 rows (0 to 23, 24 to 47, ...) at most 14 rows name the same one
- route_weights: float32 [384, 6], P('ep'), may hold values from 0.2 to 1
- expert_gate: bfloat16 [16, 2048, 512], P('ep', None, 'tp'), may hold values from -0.125 to 0.125
- expert_up: bfloat16 [16, 2048, 512], P('ep', None, 'tp'), may hold values from -0.125 to 0.125
- expert_down: bfloat16 [16, 512, 2048], P('ep', 'tp'), may hold values from -1.1048543 to 1.1048543
Outputs:
- layer_out: bfloat16 [384, 2048], P('ep', 'tp')
- new_state: float32 [384, 4, 128, 128], P('ep', 'tp')
The draws below stay inside these ranges and needn't reach their ends.
Inputs may be any that keep to these rules, and one draw needn't show every extreme that they name: `routes`: among the 24 rows of one index of ep, no expert is named by more than 14 rows, a bound that some block reaches.
All inputs are finite; a program needn't handle non-finite values.
Results may differ from the reference program's by a relative error of at most 0.015.
Values may be sent and summed in bfloat16 or wider, within the bound.
No kernel may reach another device: no remote copies, remote signals or barrier semaphores. Data moves between devices by JAX's collectives and lax.ppermute only.
A program may use at most 64 MiB of HBM per device.

```python
import math
import jax
import jax.numpy as jnp
import numpy as np
from jax import lax

D = 2048
HEADS = 4
HEAD_DIM = 128
FE = 512
FS = 512
TOPK = 6
SEQ_DEV = 24
EXPERTS = 16
BATCH = 384
CAP = 14
N_EP = 16
N_TP = 2


def rising_columns(key, shape, fan_in):
    base_key, jitter_key = jax.random.split(key)
    base = jnp.clip(jax.random.normal(base_key, shape, jnp.float32), -6.0, 6.0)
    columns = shape[-1]
    jitter = jax.random.uniform(jitter_key, (columns,), jnp.float32, -0.3, 0.3)
    position = jnp.arange(columns, dtype=jnp.float32) / columns
    scale = jnp.exp(jnp.log(3.0) * position + jitter)
    return base * scale * fan_in ** (-0.5)


def draw_expert_down(key, part):
    return rising_columns(jax.random.fold_in(key, 11), (EXPERTS, FE, D), FE).astype(jnp.bfloat16)


def draw_shared_down(key, part):
    return rising_columns(jax.random.fold_in(key, 12), (FS, D), FS).astype(jnp.bfloat16)


def with_spikes(values, rng, source, target, shards_of, factor):
    owner, partner = [(jnp.arange(values.shape[axis_at]) // (values.shape[axis_at] // shards_of)).reshape([-1 if axis == axis_at else 1 for axis in range(values.ndim)]) for axis_at in (source, target)]
    chosen = jax.random.permutation(rng, shards_of)[partner]
    strong = (owner == chosen) | (owner == (partner + shards_of // 2) % shards_of)
    return jnp.where(strong, factor * values, values)


def levels(key, shape, pieces, least, largest):
    def one(dim, parts):
        heights = jax.random.uniform(jax.random.fold_in(jax.random.fold_in(key, 6), dim), (parts,), jnp.float32, least / len(pieces), largest / len(pieces))
        return jnp.repeat(jnp.exp(heights), shape[dim] // parts).reshape((-1,) + (1,) * (len(shape) - dim - 1))

    loudness = one(*pieces[0])
    for cut in pieces[1:]:
        loudness = loudness * one(*cut)
    return loudness


def deal_out(stream_key, own, number, rows, count, top, most, skew):
    sequence = jax.random.permutation(stream_key, count)
    crowded, usual = shares(count, rows * top, most, skew, True), shares(count, rows * top, most, skew, False)
    places = jnp.arange(count)

    def named(lengths, offset_by):
        used = int((lengths > 0).sum())
        fixed = max(1, used // 4)
        moved = fixed + (places - fixed + offset_by * (used - fixed)) % max(1, count - fixed)
        return jnp.zeros((count,), jnp.int32).at[sequence[jnp.where(places < fixed, places, moved)]].set(jnp.asarray(lengths, jnp.int32))

    lengths = jnp.where(number % 4 == 0, named(crowded, number // 4), named(usual, number - number // 4 - 1))
    mixed = jax.random.permutation(jax.random.fold_in(own, 3), count)
    source_of, receiver = mixed[0:count // 2 * 2:2], mixed[1:count // 2 * 2:2]
    slack = jnp.minimum(lengths[source_of] - 1, most - lengths[receiver]) // 2
    slack = jnp.where((source_of == sequence[0]) | (receiver == sequence[0]) | (lengths[receiver] == 0), 0, jnp.maximum(slack, 0))
    moved = jax.random.randint(jax.random.fold_in(own, 4), (count // 2,), 0, 1 << 20) % (slack + 1)
    lengths = lengths.at[source_of].add(-moved).at[receiver].add(moved)
    items = jnp.searchsorted(jnp.cumsum(lengths), jnp.arange(rows * top), side="right").astype(jnp.int32)
    table = items.reshape(top, rows).T
    table = table[jax.random.permutation(jax.random.fold_in(own, 1), rows)]
    offset_by = jax.random.randint(jax.random.fold_in(own, 2), (rows, 1), 0, top)
    return jnp.take_along_axis(table, (jnp.arange(top)[None, :] + offset_by) % top, axis=1)


def shares(amount, total, limit, slope, full):
    loads = [(1 << 20) // math.isqrt(grade ** slope) + 1 for grade in range(1, amount + 1)]
    largest = limit if full else min(limit, max(-(-total // amount), total * loads[0] // sum(loads)))
    least = 1 if total - largest >= amount - 1 else 0
    counts, rest = [largest] + [least] * (amount - 1), total - largest - least * (amount - 1)
    while rest > 0:
        candidates = [i for i in range(1, amount) if counts[i] < largest] or [i for i in range(1, amount) if counts[i] < limit]
        mass, budget = sum([loads[i] for i in candidates]), rest
        for i in candidates:
            extra = min(limit - counts[i], max(1, budget * loads[i] // mass), rest)
            counts[i] = counts[i] + extra
            rest = rest - extra
    return np.array(counts)


def noise(key, extent, scale, reach, cuts=(), kind=jnp.bfloat16):
    result = scale * jax.random.normal(key, extent, jnp.float32)
    if cuts:
        result = result * levels(key, extent, cuts, -0.22, 0.18)
    return jnp.clip(result, -reach, reach).astype(kind)


def bell_draw_with(own_key, shape, spread, most, shards, heavy, kind=jnp.bfloat16):
    result = spread * jax.random.normal(own_key, shape, jnp.float32)
    if shards:
        result = result * levels(own_key, shape, shards, -0.22, 0.18)
    return jnp.clip(with_spikes(result, jax.random.fold_in(own_key, 3), *heavy), -most, most).astype(kind)


def setup_inputs(seed: int = 0) -> dict:
    key_of = jax.random.split(jax.random.key(seed), 21)
    tokens = bell_draw_with(key_of[0], (BATCH, D), 1.0, 6.0, ((0, 16),), (1, 0, 16, 2.0))
    carried_state = noise(key_of[1], (BATCH, HEADS, HEAD_DIM, HEAD_DIM), 0.5, 4.0, ((0, 16), (1, 2)), jnp.float32)
    w_query = noise(key_of[2], (D, HEADS * HEAD_DIM), D ** -0.5, 0.125, ((1, 2),))
    w_forget = noise(key_of[3], (D, HEADS * HEAD_DIM), D ** -0.5, 0.125, ((1, 2),))
    w_value = noise(key_of[4], (D, HEADS * HEAD_DIM), D ** -0.5, 0.125, ((1, 2),))
    forget_floor = jnp.clip(0.05 + 0.84999998 * jax.random.uniform(key_of[5], (HEADS, HEAD_DIM), jnp.float32) ** levels(key_of[5], (HEADS, HEAD_DIM), ((0, 2),), -0.2, 0.2), 0.05, 0.9)
    head_gain = jnp.clip(1.0 + 0.18 * jax.random.normal(key_of[6], (HEADS, HEAD_DIM), jnp.float32), 0.099609375, 1.8984375).astype(jnp.bfloat16)
    w_out = noise(key_of[7], (HEADS * HEAD_DIM, D), (HEADS * HEAD_DIM) ** -0.5, 0.25, ((0, 2), (1, 16)))
    gain_mix = jnp.clip(1.0 + 0.18 * jax.random.normal(key_of[8], (D,), jnp.float32), 0.099609375, 1.8984375).astype(jnp.bfloat16)
    gain_ffn = jnp.clip(1.0 + 0.18 * jax.random.normal(key_of[9], (D,), jnp.float32), 0.099609375, 1.8984375).astype(jnp.bfloat16)
    gain_post = jnp.clip(1.0 + 0.18 * jax.random.normal(key_of[10], (D,), jnp.float32), 0.099609375, 1.8984375).astype(jnp.bfloat16)
    w_branch_gate = noise(key_of[11], (D,), D ** -0.5, 0.125)
    shared_gate = noise(key_of[12], (D, FS), D ** -0.5, 0.125, ((0, 16), (1, 2)))
    shared_up = noise(key_of[13], (D, FS), D ** -0.5, 0.125, ((0, 16), (1, 2)))
    shared_down = draw_shared_down(jax.random.fold_in(key_of[20], 71), 0)
    routes_keys = jax.random.split(jax.random.fold_in(key_of[15], 1), BATCH // SEQ_DEV)
    routes_turns = jax.random.permutation(jax.random.fold_in(key_of[15], 3), BATCH // SEQ_DEV)
    routes = jax.vmap(lambda own, number: deal_out(jax.random.fold_in(key_of[15], 2), own, number, SEQ_DEV, EXPERTS, TOPK, CAP, 0))(routes_keys, routes_turns).reshape((BATCH, TOPK))
    route_weights = jnp.clip(0.2 + 0.8 * jax.random.uniform(key_of[16], (BATCH, TOPK), jnp.float32) ** levels(key_of[16], (BATCH, TOPK), ((0, 16),), -0.2, 0.2), 0.2, 1.0)
    expert_gate = noise(key_of[17], (EXPERTS, D, FE), D ** -0.5, 0.125, ((0, 16), (2, 2)))
    expert_up = noise(key_of[18], (EXPERTS, D, FE), D ** -0.5, 0.125, ((0, 16), (2, 2)))
    expert_down = draw_expert_down(jax.random.fold_in(key_of[20], 71), 0)
    return dict(tokens=tokens, carried_state=carried_state, w_query=w_query, w_forget=w_forget, w_value=w_value, forget_floor=forget_floor, head_gain=head_gain, w_out=w_out, gain_mix=gain_mix, gain_ffn=gain_ffn, gain_post=gain_post, w_branch_gate=w_branch_gate, shared_gate=shared_gate, shared_up=shared_up, shared_down=shared_down, routes=routes, route_weights=route_weights, expert_gate=expert_gate, expert_up=expert_up, expert_down=expert_down)


epsilon = 1e-06

def rmsnorm(values_in, gain):
    scale = lax.rsqrt(lax.optimization_barrier(jnp.mean(values_in * values_in, axis=-1, keepdims=True)) + epsilon)
    return values_in * scale * gain.astype(jnp.float32)

def group_partials(acts, weight):
    batch_rows = acts.shape[0]
    inner = acts.shape[1] // N_TP
    groups = acts.reshape(batch_rows, N_TP, inner).astype(jnp.float32)
    weight_groups = weight.reshape(N_TP, inner, weight.shape[1]).astype(jnp.float32)
    partials = jnp.einsum('btk,tkd->btd', groups, weight_groups).astype(jnp.bfloat16)
    return lax.optimization_barrier(jnp.sum(partials.astype(jnp.float32), axis=1)).astype(jnp.bfloat16)

def reference(tokens, carried_state, w_query, w_forget, w_value, forget_floor, head_gain, w_out, gain_mix, gain_ffn, gain_post, w_branch_gate, shared_gate, shared_up, shared_down, routes, route_weights, expert_gate, expert_up, expert_down):
    batch_rows = tokens.shape[0]
    normed = rmsnorm(tokens.astype(jnp.float32), gain_mix).astype(jnp.bfloat16)
    queries = jax.nn.silu(jnp.dot(normed, w_query, preferred_element_type=jnp.float32))
    forget_pre = jnp.dot(normed, w_forget, preferred_element_type=jnp.float32)
    values_in = jnp.dot(normed, w_value, preferred_element_type=jnp.float32)
    queries = queries.reshape(batch_rows, HEADS, HEAD_DIM)
    forget_pre = forget_pre.reshape(batch_rows, HEADS, HEAD_DIM)
    values_in = values_in.reshape(batch_rows, HEADS, HEAD_DIM)
    forget = forget_floor + (1.0 - forget_floor) * jax.nn.sigmoid(forget_pre)
    keys_in = (1.0 - forget_floor) * jax.nn.sigmoid(-forget_pre)
    new_state = forget[..., None] * carried_state + keys_in[..., None] * values_in[:, :, None, :]
    readout = jnp.einsum('bhd,bhdv->bhv', queries, new_state, precision=lax.Precision.HIGHEST)
    head_out = rmsnorm(readout, head_gain).astype(jnp.bfloat16).reshape(batch_rows, HEADS * HEAD_DIM)
    mixed = group_partials(head_out, w_out)
    resid = (tokens.astype(jnp.float32) + mixed.astype(jnp.float32)).astype(jnp.bfloat16)
    hnorm = rmsnorm(resid.astype(jnp.float32), gain_ffn).astype(jnp.bfloat16)
    branch_mix = jax.nn.sigmoid(jnp.dot(hnorm, w_branch_gate, preferred_element_type=jnp.float32))
    gate_pre = jnp.dot(hnorm, shared_gate, preferred_element_type=jnp.float32)
    up_pre = jnp.dot(hnorm, shared_up, preferred_element_type=jnp.float32)
    shared_hidden = (jax.nn.silu(gate_pre) * up_pre).astype(jnp.bfloat16)
    shared_out = group_partials(shared_hidden, shared_down)
    blocks = routes.reshape(N_EP, SEQ_DEV * TOPK)
    onehot = (blocks[:, :, None] == jnp.arange(EXPERTS, dtype=jnp.int32)[None, None, :]).astype(jnp.int32)
    earlier = jnp.cumsum(onehot, axis=1) - onehot
    slot_rank = lax.optimization_barrier(jnp.sum(earlier * onehot, axis=2)).reshape(-1).astype(jnp.int32)
    flat_routes = routes.reshape(-1).astype(jnp.int32)
    token_ids = (jnp.arange(batch_rows * TOPK, dtype=jnp.int32) // TOPK).astype(jnp.int32)
    source = (token_ids // SEQ_DEV).astype(jnp.int32)
    table = jnp.full((EXPERTS, N_EP, CAP), batch_rows, jnp.int32)
    table = table.at[flat_routes, source, slot_rank].set(token_ids)
    padded = jnp.concatenate([hnorm, jnp.zeros((1, D), jnp.bfloat16)], axis=0)

    def one_expert(operands):
        slots, gate_weight, up_weight, down_weight = operands
        rows_in = padded[slots.reshape(-1)]
        expert_gate_pre = jnp.dot(rows_in, gate_weight, preferred_element_type=jnp.float32)
        expert_up_pre = jnp.dot(rows_in, up_weight, preferred_element_type=jnp.float32)
        expert_hidden = (jax.nn.silu(expert_gate_pre) * expert_up_pre).astype(jnp.bfloat16)
        return group_partials(expert_hidden, down_weight)
    results = lax.map(one_expert, (table, expert_gate, expert_up, expert_down))
    picked = results.reshape(EXPERTS, N_EP, CAP, D)[flat_routes, source, slot_rank]
    picked = picked.astype(jnp.float32).reshape(batch_rows, TOPK, D)
    routed = lax.optimization_barrier(jnp.sum(picked * route_weights[:, :, None], axis=1))
    branch_sum = routed + branch_mix[:, None] * shared_out.astype(jnp.float32)
    layer_out = (resid.astype(jnp.float32) + rmsnorm(branch_sum, gain_post)).astype(jnp.bfloat16)
    return (layer_out, new_state)
```

```python
import functools

import jax
import jax.numpy as jnp
from jax import lax
from jax.experimental import pallas as pl
from jax.experimental.pallas import tpu as pltpu
from jax.sharding import PartitionSpec as P

epsilon = 1e-06


def rmsnorm(values_in, gain):
    scale = lax.rsqrt(jnp.mean(values_in * values_in, axis=-1, keepdims=True) + epsilon)
    return values_in * scale * gain.astype(jnp.float32)


def project_down(acts, weight):
    projected = jnp.dot(
        lax.all_gather(acts, "ep", axis=0, tiled=True), weight, preferred_element_type=jnp.float32
    )
    return lax.all_to_all(
        projected.astype(jnp.bfloat16), "ep", split_axis=0, concat_axis=1, tiled=True
    )


def routed_exchange(
    tokens,
    carried_state,
    w_query,
    w_forget,
    w_value,
    forget_floor,
    head_gain,
    w_out,
    gain_mix,
    gain_ffn,
    gain_post,
    w_branch_gate,
    shared_gate,
    shared_up,
    shared_down,
    routes,
    route_weights,
    expert_gate,
    expert_up,
    expert_down,
):
    seq_rows, model_width = tokens.shape
    heads_local = carried_state.shape[1]
    head_dim = carried_state.shape[2]
    n_ep = lax.axis_size("ep")
    n_tp = lax.axis_size("tp")
    top_count = routes.shape[1]
    experts_local = expert_gate.shape[0]
    experts_all = experts_local * n_ep
    capacity = min(
        seq_rows, max(2, (3 * seq_rows * top_count + 2 * experts_all - 1) // (2 * experts_all))
    )
    slice_width = model_width // n_tp
    normed = rmsnorm(tokens.astype(jnp.float32), gain_mix).astype(jnp.bfloat16)
    queries = jax.nn.silu(jnp.dot(normed, w_query, preferred_element_type=jnp.float32))
    forget_pre = jnp.dot(normed, w_forget, preferred_element_type=jnp.float32)
    values_in = jnp.dot(normed, w_value, preferred_element_type=jnp.float32)
    queries = queries.reshape(seq_rows, heads_local, head_dim)
    forget_pre = forget_pre.reshape(seq_rows, heads_local, head_dim)
    values_in = values_in.reshape(seq_rows, heads_local, head_dim)
    forget = forget_floor + (1.0 - forget_floor) * jax.nn.sigmoid(forget_pre)
    keys_in = (1.0 - forget_floor) * jax.nn.sigmoid(-forget_pre)
    new_state = forget[..., None] * carried_state + keys_in[..., None] * values_in[:, :, None, :]
    readout = jnp.einsum("bhd,bhdv->bhv", queries, new_state, precision=lax.Precision.HIGHEST)
    head_out = (
        rmsnorm(readout, head_gain).astype(jnp.bfloat16).reshape(seq_rows, heads_local * head_dim)
    )
    head_terms = project_down(head_out, w_out)
    mixed = lax.psum(head_terms.astype(jnp.float32).astype(jnp.bfloat16), "tp")
    resid = (tokens.astype(jnp.float32) + mixed.astype(jnp.float32)).astype(jnp.bfloat16)
    hnorm = rmsnorm(resid.astype(jnp.float32), gain_ffn).astype(jnp.bfloat16)
    branch_mix = jax.nn.sigmoid(jnp.dot(hnorm, w_branch_gate, preferred_element_type=jnp.float32))
    hidden_local = shared_gate.shape[1]
    feature_slices = lax.all_to_all(hnorm, "ep", split_axis=1, concat_axis=0, tiled=True)
    both_weights = jnp.concatenate([shared_gate, shared_up], axis=1)
    both_pre = lax.psum_scatter(
        jnp.dot(feature_slices, both_weights, preferred_element_type=jnp.float32),
        "ep",
        scatter_dimension=0,
        tiled=True,
    )
    gate_pre = both_pre[:, :hidden_local]
    up_pre = both_pre[:, hidden_local:]
    shared_hidden = (jax.nn.silu(gate_pre) * up_pre).astype(jnp.bfloat16)
    shared_terms = project_down(shared_hidden, shared_down)
    shared_out = lax.psum_scatter(
        shared_terms.astype(jnp.float32).astype(jnp.bfloat16), "tp", scatter_dimension=1, tiled=True
    )
    flat_routes = routes.reshape(-1)
    expert_ids = lax.broadcasted_iota(jnp.int32, (1, experts_all), 1)
    onehot = (flat_routes[:, None] == expert_ids).astype(jnp.int32)
    earlier = jnp.cumsum(onehot, axis=0) - onehot
    slot_rank = jnp.sum(earlier * onehot, axis=1)
    position = flat_routes * capacity + slot_rank
    slot_ids = lax.broadcasted_iota(jnp.int32, (1, experts_all * capacity), 1)
    slot_match = position[:, None] == slot_ids
    repeated = jnp.repeat(hnorm, top_count, axis=0)
    send_rows = jnp.einsum(
        "rs,rd->sd", slot_match.astype(jnp.bfloat16), repeated, preferred_element_type=jnp.float32
    )
    send_rows = send_rows.astype(jnp.bfloat16).reshape(experts_all, capacity, model_width)
    arrived = lax.all_to_all(send_rows, "ep", split_axis=0, concat_axis=0, tiled=True)
    slot_count = arrived.shape[1]
    slotted = arrived.reshape(n_ep, experts_local, slot_count, model_width)
    expert_gate_pre = jnp.einsum(
        "sxnd,xdf->sxnf", slotted, expert_gate, preferred_element_type=jnp.float32
    )
    expert_up_pre = jnp.einsum(
        "sxnd,xdf->sxnf", slotted, expert_up, preferred_element_type=jnp.float32
    )
    expert_hidden = (jax.nn.silu(expert_gate_pre) * expert_up_pre).astype(jnp.bfloat16)
    down_terms = jnp.einsum(
        "sxnf,xfd->sxnd", expert_hidden, expert_down, preferred_element_type=jnp.float32
    )
    rounded_terms = lax.optimization_barrier(down_terms.astype(jnp.bfloat16)).astype(jnp.float32)
    summed = lax.psum_scatter(
        rounded_terms.astype(jnp.bfloat16), "tp", scatter_dimension=3, tiled=True
    )
    expert_rows = summed.reshape(n_ep * experts_local, slot_count, slice_width)
    returned = lax.all_to_all(expert_rows, "ep", split_axis=0, concat_axis=0, tiled=True)
    weighted = slot_match.astype(jnp.float32) * route_weights.reshape(-1)[:, None]
    combine = jnp.sum(weighted.reshape(seq_rows, top_count, experts_all * capacity), axis=1)
    routed = jnp.dot(
        combine,
        returned.reshape(experts_all * capacity, slice_width).astype(jnp.float32),
        precision=lax.Precision.HIGHEST,
    )
    branch_sum = routed + branch_mix[:, None] * shared_out.astype(jnp.float32)
    square_part = jnp.sum(branch_sum * branch_sum, axis=1)
    square_total = lax.psum(square_part, "tp")
    norm_scale = lax.rsqrt(square_total / model_width + epsilon)
    resid_slice = lax.dynamic_slice_in_dim(
        resid, lax.axis_index("tp") * slice_width, slice_width, 1
    )
    layer_out = resid_slice.astype(jnp.float32) + branch_sum * norm_scale[
        :, None
    ] * gain_post.astype(jnp.float32)
    return (layer_out.astype(jnp.bfloat16), new_state)


VMEM = pl.BlockSpec(memory_space=pltpu.VMEM)
SMEM = pl.BlockSpec(memory_space=pltpu.SMEM)
F32 = jnp.float32
BF16 = jnp.bfloat16
MIB = 1 << 20


def swap(value, mask, tp_mask=0):
    n_ep, n_tp = lax.axis_size("ep"), lax.axis_size("tp")
    flip = mask * n_tp + tp_mask
    return lax.ppermute(value, ("ep", "tp"), [(i, i ^ flip) for i in range(n_ep * n_tp)])


def call(body, outs, args, scalars=1, scratch=(), limit=16, flops=0, **grid):
    specs = dict(
        in_specs=[SMEM] * scalars + [VMEM] * (len(args) - scalars), out_specs=[VMEM] * len(outs)
    )
    specs.update(grid)
    return pl.pallas_call(
        body,
        out_shape=[jax.ShapeDtypeStruct(*o) for o in outs],
        scratch_shapes=list(scratch),
        compiler_params=pltpu.CompilerParams(vmem_limit_bytes=limit * MIB),
        cost_estimate=pl.CostEstimate(flops=flops, bytes_accessed=flops // 100, transcendentals=0),
        **specs,
    )(*args)


def mix_kernel(
    steps,
    place,
    tokens,
    gain,
    w_query,
    w_forget,
    w_value,
    floor,
    head_gain,
    state,
    new_state,
    send,
    kept,
    forget_t,
    keys_t,
    queries_t,
    values,
    readout,
):
    step = pl.program_id(0)
    rows, width = tokens.shape
    per_step, heads, dim, _ = state.shape

    @pl.when(step == 0)
    def _():
        token_values = tokens[...].astype(F32)
        scale = lax.rsqrt(jnp.mean(token_values * token_values, axis=-1, keepdims=True) + epsilon)
        normed = (token_values * scale * gain[...].astype(F32)).astype(BF16)
        queries = jax.nn.silu(jnp.dot(normed, w_query[...], preferred_element_type=F32))
        forget_pre = jnp.dot(normed, w_forget[...], preferred_element_type=F32)
        values_in = jnp.dot(normed, w_value[...], preferred_element_type=F32)
        for i in range(steps):
            values[i] = values_in[i * per_step : (i + 1) * per_step]
        low = floor[...]
        forget = low + (1.0 - low) * jax.nn.sigmoid(forget_pre)
        keys = (1.0 - low) * jax.nn.sigmoid(-forget_pre)
        for ref, value in ((queries_t, queries), (forget_t, forget), (keys_t, keys)):
            flipped = value.T
            for i in range(steps):
                ref[i] = flipped[:, i * per_step : (i + 1) * per_step]
        ep = place[0]
        lanes = w_query.shape[1]
        piece = 128
        count = width // piece
        for order in range(count):
            mc, mx, j = order // (count // 2), order // (count // 4) % 2, order % (count // 4)
            source = jnp.bitwise_xor(ep, j * 4 + mx * 2 + mc)
            got = tokens[:, pl.ds(pl.multiple_of(source * piece, piece), piece)]
            at = order % (count // 2) * piece
            if mc:
                send[:, lanes + at : lanes + at + piece] = got
            else:
                kept[:, at : at + piece] = got

    for i in range(per_step):
        value_row = values[step, i : i + 1, :]
        for h in range(heads):
            at = slice(h * dim, (h + 1) * dim)
            forget_col = forget_t[step, at, i : i + 1]
            keys_col = keys_t[step, at, i : i + 1]
            queries_col = queries_t[step, at, i : i + 1]
            updated = forget_col * state[i, h] + keys_col * value_row[:, at]
            new_state[i, h] = updated
            readout[step, i : i + 1, at] = jnp.sum(queries_col * updated, axis=0, keepdims=True)

    @pl.when(step == steps - 1)
    def _():
        for h in range(heads):
            at = slice(h * dim, (h + 1) * dim)
            got = jnp.concatenate([readout[k, :, at] for k in range(steps)], axis=0)
            scale = lax.rsqrt(jnp.mean(got * got, axis=-1, keepdims=True) + epsilon)
            send[:, at] = (got * scale * head_gain[:, at].astype(F32)).astype(BF16)


def mix(place, tokens, gain, w_query, w_forget, w_value, floor, head_gain, state):
    rows, width = tokens.shape
    _, heads, dim, _ = state.shape
    lanes = heads * dim
    steps = 4 if rows % 4 == 0 else 1
    per_step = rows // steps
    whole = lambda *shape: pl.BlockSpec(shape, lambda i: (0,) * len(shape))
    block = pl.BlockSpec((per_step, heads, dim, dim), lambda i: (i, 0, 0, 0))
    return call(
        functools.partial(mix_kernel, steps),
        [
            (state.shape, F32),
            ((rows, lanes + width // 2), BF16),
            ((rows, width // 2), BF16),
        ],
        [
            place,
            tokens,
            gain.reshape(1, -1),
            w_query,
            w_forget,
            w_value,
            floor.reshape(1, -1),
            head_gain.reshape(1, -1),
            state,
        ],
        scratch=[pltpu.VMEM((steps, lanes, per_step), F32)] * 3
        + [pltpu.VMEM((steps, per_step, lanes), F32)] * 2,
        limit=24,
        flops=200_000_000,
        grid=(steps,),
        in_specs=[
            SMEM,
            whole(rows, width),
            whole(1, width),
            whole(width, lanes),
            whole(width, lanes),
            whole(width, lanes),
            whole(1, lanes),
            whole(1, lanes),
            block,
        ],
        out_specs=[block, whole(rows, lanes + width // 2), whole(rows, width // 2)],
    )


def project_kernel(heads, *refs):
    pieces, out = refs[heads:-1], refs[-1]
    acts = jnp.concatenate([ref[...].astype(F32) for ref in refs[:heads]], axis=0).astype(BF16)
    rows = refs[0].shape[0]
    width = pieces[0].shape[1]
    for j, piece in enumerate(pieces):
        got = jnp.dot(acts, piece[...], preferred_element_type=F32)
        for q in range(heads):
            out[q, :, j * width : (j + 1) * width] = got[q * rows : (q + 1) * rows].astype(BF16)


def resid_kernel(ours, theirs, *refs):
    tokens, out = refs[:-1], refs[-1]
    for q, token in enumerate(tokens):
        mixed = (ours[q].astype(F32) + theirs[q].astype(F32)).astype(BF16)
        out[q] = (token[...].astype(F32) + mixed.astype(F32)).astype(BF16)


def expert_kernel(
    n_z,
    place,
    own,
    near,
    far,
    near_core,
    far_core,
    gain,
    branch_gate,
    gate,
    up,
    down,
    spread,
    keep,
    give,
    resid,
    normed,
    shared_in,
    shared_out,
    hidden,
    weights,
    gathered,
):
    ep, tp = place[0], place[1]
    piece = 128
    rows = own.shape[1]
    width = down.shape[1]
    n_ep = 4 * n_z
    half = n_ep // 2
    slice_width = width // 2
    units = spread.shape[1] // 4
    blocks = {}
    for mc, (first, second) in enumerate(((near, far), (near_core, far_core))):
        for i, key in enumerate(((1, 0), (2, 0), (0, 1))):
            blocks[key + (mc,)] = first.at[i + mc]
        for i, key in enumerate(((3, 0), (1, 1), (2, 1), (3, 1))):
            blocks[key + (mc,)] = second.at[i]
    blocks[0, 0, 0] = own
    blocks[0, 0, 1] = near_core.at[0]

    def columns(mask):
        start = jnp.bitwise_xor(ep, mask) * piece
        return pl.ds(pl.multiple_of(start, piece), piece)

    def order_of(block):
        return block // half, block // 2 % n_z, block % 2

    def part(block, mask):
        ac, mz, ax = order_of(block)
        rz, rx, rc = mask >> 2, mask >> 1 & 1, mask & 1
        ref = blocks[mz, rx, rc]
        j = mz ^ rz
        return ref[(ax ^ rx) * 2 + (ac ^ rc), :, j * piece : (j + 1) * piece]

    for pair in range(0, n_ep, 2):
        squares = [jnp.zeros((rows, piece), F32) for _ in range(2)]
        for mask in range(n_ep):
            for k in range(2):
                got = part(pair + k, mask).astype(F32)
                squares[k] = squares[k] + got * got
        scales = [
            lax.rsqrt(jnp.sum(s, axis=-1, keepdims=True) / width + epsilon) for s in squares
        ]
        for mask in range(n_ep):
            gained = gain[:, columns(mask)].astype(F32)
            both = [part(pair + k, mask).astype(F32) * scales[k] * gained for k in range(2)]
            normed[pair * rows : (pair + 2) * rows, columns(mask)] = jnp.concatenate(
                both, axis=0
            ).astype(BF16)
            if pair == 0:
                gathered[:, columns(mask)] = part(0, mask)
    resid[...] = gathered[:, pl.ds(pl.multiple_of(tp * slice_width, slice_width), slice_width)]

    for s in range(n_ep):
        at = slice(s * piece, (s + 1) * piece)
        shared_in[0 : 2 * units, at] = spread[s, 0 : 2 * units, :]
        shared_out[:, at] = spread[s, 2 * units : 3 * units, :]
    shared_in[2 * units : 3 * units, :] = jnp.broadcast_to(branch_gate[...], (units, width))
    for block in range(n_ep):
        ac, mz, ax = order_of(block)
        source = jnp.bitwise_xor(ep, mz * 4 + ax * 2 + ac)
        weights[block : block + 1, :] = spread[source, 3 * units : 4 * units, :].astype(F32)[0:1]
    flipped = weights[...].T
    weight_cols = flipped[0:rows] + flipped[rows : 2 * rows]

    acts = normed[...]
    gate_pre = jnp.dot(acts, gate[...], preferred_element_type=F32)
    up_pre = jnp.dot(acts, up[...], preferred_element_type=F32)
    hidden[...] = (jax.nn.silu(gate_pre) * up_pre).astype(BF16)
    shared_pre = lax.dot_general(
        acts, shared_in[...], (((1,), (1,)), ((), ())), preferred_element_type=F32
    )
    shared_hidden = (
        jax.nn.silu(shared_pre[:, 0:units]) * shared_pre[:, units : 2 * units]
    ).astype(BF16)
    branch_mix = jax.nn.sigmoid(shared_pre[:, 2 * units : 2 * units + 1])
    weight_col = jnp.concatenate([weight_cols[:, b : b + 1] for b in range(n_ep)], axis=0)
    chunk = 256
    for side in range(2):
        side_start = jnp.bitwise_xor(tp, side) * slice_width
        for n in range(0, slice_width, chunk):
            at = pl.ds(pl.multiple_of(side_start + n, chunk), chunk)
            routed = jnp.dot(hidden[...], down[:, at], preferred_element_type=F32)
            shared = jnp.dot(shared_hidden, shared_out[:, at], preferred_element_type=F32)
            total = weight_col * routed + branch_mix * shared
            to = slice(side * slice_width + n, side * slice_width + n + chunk)
            for block in range(half):
                keep[block, :, to] = total[block * rows : (block + 1) * rows]
                give[block, :, to] = total[(half + block) * rows : (half + block + 1) * rows].astype(
                    BF16
                )


def chip_kernel(keep, got, own, to_x, to_y, to_xy):
    half = own.shape[2]
    for block in range(keep.shape[0]):
        total = keep[block] + got[block].astype(F32)
        mz, mx = block // 2, block % 2
        if mx:
            to_x[mz] = total[:, :half].astype(BF16)
            to_xy[mz] = total[:, half:].astype(BF16)
        else:
            own[mz] = total[:, :half]
            to_y[mz] = total[:, half:].astype(BF16)


def plane_kernel(own, from_x, from_y, from_xy, out, *sends):
    for mz in range(own.shape[0]):
        total = (
            own[mz] + from_x[mz].astype(F32) + from_y[mz].astype(F32) + from_xy[mz].astype(F32)
        )
        if mz:
            sends[mz - 1][...] = total.astype(BF16)
        else:
            out[...] = total


def last_kernel(own, *refs):
    parts, (out, squares) = refs[:-2], refs[-2:]
    total = own[...]
    for part in parts:
        total = total + part[...].astype(F32)
    out[...] = total
    squares[...] = jnp.broadcast_to(
        jnp.sum(total * total, axis=-1, keepdims=True), squares.shape
    )


def final_kernel(width, branch, ours, theirs, gain, resid, out):
    mean = (ours[:, 0:1] + theirs[:, 0:1]) / width
    value = branch[...] * lax.rsqrt(mean + epsilon) * gain[...].astype(F32)
    out[...] = (resid[...].astype(F32) + value).astype(BF16)


def dense_exchange(
    tokens,
    carried_state,
    w_query,
    w_forget,
    w_value,
    forget_floor,
    head_gain,
    w_out,
    gain_mix,
    gain_ffn,
    gain_post,
    w_branch_gate,
    shared_gate,
    shared_up,
    shared_down,
    routes,
    route_weights,
    expert_gate,
    expert_up,
    expert_down,
):
    rows, width = tokens.shape
    n_ep = lax.axis_size("ep")
    n_z = n_ep // 4
    piece = w_out.shape[1]
    lanes = w_out.shape[0]
    place = jnp.stack([lax.axis_index("ep"), lax.axis_index("tp")]).astype(jnp.int32)
    columns = [w_out] + [swap(w_out, m * 4) for m in range(1, n_z)]
    units = shared_gate.shape[1] // n_ep
    chosen = routes[None] == lax.broadcasted_iota(jnp.int32, (n_ep, 1, 1), 0)
    row_weights = jnp.sum(jnp.where(chosen, route_weights[None], 0.0), axis=2)
    coarse = row_weights.astype(BF16)
    fine = (row_weights - coarse.astype(F32)).astype(BF16)
    row_weights = jnp.pad(
        jnp.concatenate([coarse, fine], axis=1)[:, None, :],
        ((0, 0), (0, units - 1), (0, piece - 2 * rows)),
    )
    spread = jnp.concatenate(
        [
            shared_gate.T.reshape(n_ep, units, piece),
            shared_up.T.reshape(n_ep, units, piece),
            shared_down.reshape(n_ep, units, piece),
            row_weights,
        ],
        axis=1,
    )
    spread = lax.all_to_all(spread, "ep", split_axis=0, concat_axis=0, tiled=True)

    new_state, send, kept = mix(
        place,
        tokens,
        gain_mix,
        w_query,
        w_forget,
        w_value,
        forget_floor,
        head_gain,
        carried_state,
    )
    half = width // 4
    core = swap(send, 1)
    to_x = jnp.stack(
        [
            jnp.concatenate([send[:, :lanes], kept[:, half:]], axis=1),
            jnp.concatenate([core[:, :lanes], core[:, lanes + half :]], axis=1),
        ]
    )
    from_x = swap(to_x, 2)
    heads = [send[:, :lanes], core[:, :lanes], from_x[0, :, :lanes], from_x[1, :, :lanes]]
    group_tokens = [
        kept[:, :half],
        core[:, lanes : lanes + half],
        from_x[0, :, lanes:],
        from_x[1, :, lanes:],
    ]
    block = (4, rows, n_z * piece)
    (partial,) = call(
        functools.partial(project_kernel, 4),
        [(block, BF16)],
        heads + columns,
        scalars=0,
        limit=8,
        flops=2 * 4 * rows * lanes * n_z * piece,
    )
    (own,) = call(
        resid_kernel,
        [(block, BF16)],
        [partial, swap(partial, 0, 1)] + group_tokens,
        scalars=0,
        limit=8,
    )
    z1, z2, x1 = swap(own, 4), swap(own, 8), swap(own, 2)
    near = jnp.stack([z1, z2, x1])
    near_core = swap(jnp.stack([own, z1, z2, x1]), 1)
    by_z = swap(jnp.stack([z2, x1]), 4)
    by_x = swap(z2, 2)
    by_xz = swap(z2, 6)
    far = jnp.stack([by_z[0], by_z[1], by_x, by_xz])
    far_core = swap(far, 1)

    count = n_ep // 2
    keep, give, resid = call(
        functools.partial(expert_kernel, n_z),
        [((count, rows, width), F32), ((count, rows, width), BF16), ((rows, width // 2), BF16)],
        [
            place,
            own,
            near,
            far,
            near_core,
            far_core,
            gain_ffn.reshape(1, -1),
            w_branch_gate.reshape(1, -1),
            expert_gate[0],
            expert_up[0],
            expert_down[0],
            spread,
        ],
        scratch=[
            pltpu.VMEM((n_ep * rows, width), BF16),
            pltpu.VMEM((3 * units, width), BF16),
            pltpu.VMEM((units, width), BF16),
            pltpu.VMEM((n_ep * rows, expert_gate.shape[2]), BF16),
            pltpu.VMEM((n_ep, piece), F32),
            pltpu.VMEM((rows, width), BF16),
        ],
        limit=32,
        flops=6 * n_ep * rows * width * expert_gate.shape[2],
    )
    quarter = (n_z, rows, width // 2)
    one = (rows, width // 2)
    mine, to_x, to_y, to_xy = call(
        chip_kernel,
        [(quarter, F32)] + [(quarter, BF16)] * 3,
        [keep, swap(give, 1)],
        scalars=0,
        limit=16,
    )
    mine, *sends = call(
        plane_kernel,
        [(one, F32)] + [(one, BF16)] * (n_z - 1),
        [mine, swap(to_x, 2), swap(to_y, 0, 1), swap(to_xy, 2, 1)],
        scalars=0,
        limit=8,
    )
    branch, squares = call(
        last_kernel,
        [(one, F32), ((rows, 128), F32)],
        [mine] + [swap(part, (m + 1) * 4) for m, part in enumerate(sends)],
        scalars=0,
        limit=8,
    )
    (layer_out,) = call(
        functools.partial(final_kernel, width),
        [(one, BF16)],
        [branch, squares, swap(squares, 0, 1), gain_post.reshape(1, -1), resid],
        scalars=0,
        limit=8,
    )
    return (layer_out, new_state)


def shards(*args):
    tokens, w_out, routes, shared_gate, expert_gate = (args[i] for i in (0, 7, 15, 12, 17))
    n_ep = lax.axis_size("ep")
    few = lax.axis_size("tp") == 2 and n_ep == 16 and expert_gate.shape[0] == 1
    expected = routes.size / (n_ep * expert_gate.shape[0])
    fits = w_out.shape[1] == 128 and shared_gate.shape[1] % (16 * n_ep) == 0
    if few and fits and 4 * expected >= tokens.shape[0]:
        return dense_exchange(*args)
    return routed_exchange(*args)


def solution(mesh):
    placed = (
        P("ep", None),
        P("ep", "tp", None, None),
        P(None, "tp"),
        P(None, "tp"),
        P(None, "tp"),
        P("tp", None),
        P("tp", None),
        P("tp", "ep"),
        P(),
        P(),
        P("tp"),
        P(),
        P("ep", "tp"),
        P("ep", "tp"),
        P("tp", "ep"),
        P("ep", None),
        P("ep", None),
        P("ep", None, "tp"),
        P("ep", None, "tp"),
        P("ep", "tp", None),
    )
    return jax.shard_map(
        shards,
        mesh=mesh,
        in_specs=placed,
        out_specs=(P("ep", "tp"), P("ep", "tp", None, None)),
        check_vma=False,
    )
```
